32 devices in a mesh: ep: 8 (over z, x), tp: 4 (over y, core).
Axes of the slice: x: 2, y: 2, z: 4, core: 2. Of those that a mesh axis runs over, the one named last changes fastest.
Arguments:
- queries: bfloat16 [2048, 1024], P('ep', 'tp'), may hold values from -6 to 6
- key_rows: bfloat16 [2048, 1024], P('ep', 'tp'), may hold values from -6 to 6
- value_rows: bfloat16 [2048, 1024], P('ep', 'tp'), may hold values from -6 to 6
- out_gate: bfloat16 [2048, 1024], P('ep', 'tp'), may hold values from -6 to 6
- log_decay: float32 [2048, 8], P('ep', 'tp'), may hold values from -3 to 0, as said below
- head_gain: float32 [8, 128], P('tp'), may hold values from 0.1 to 1.9
- out_weight: bfloat16 [1024, 2048], P('tp'), may hold values from -0.1875 to 0.1875
- moe_input: bfloat16 [1024, 2048], P('ep'), may hold values from -6 to 6
- moe_gain: float32 [2048], replicated, may hold values from 0.1 to 1.9
- expert_gate: bfloat16 [8, 2048, 3584], P('ep', None, 'tp'), may hold values from -0.125 to 0.125
- expert_up: bfloat16 [8, 2048, 3584], P('ep', None, 'tp'), may hold values from -0.125 to 0.125
- expert_down: bfloat16 [8, 3584, 2048], P('ep', 'tp'), may hold values from -0.125 to 0.125
- route_ids: int32 [1024, 2], P('ep'), may hold values from 0 to 7, all different within a row; in each aligned block of 128 rows (0 to 127, 128 to 255, ...) at most 64 rows name the same one
- route_weights: float32 [1024, 2], P('ep'), may hold values from 0.2 to 1
Outputs:
- mixer_out: bfloat16 [2048, 2048], P(('ep', 'tp'))
- expert_out: bfloat16 [1024, 2048], P('ep', 'tp')
The draws below stay inside these ranges and needn't reach their ends.
Inputs may be any that keep to these rules, and one draw needn't show every extreme that they name: `route_ids`: among the 2 entries of a row no expert repeats. In each aligned block of 128 rows (the rows of one index of ep) no expert is named more than 64 times, a bound that some block reaches. `log_decay`: every entry is negative.
All inputs are finite; a program needn't handle non-finite values.
Results may differ from the reference program's by a relative error of at most 0.017.
Values may be sent and summed in bfloat16 or wider, within the bound.
A program may use at most 64 MiB of HBM per device.

```python
import math
import jax
import jax.numpy as jnp
import numpy as np
from jax import lax

D = 2048
HEADS = 8
HEAD = 128
EFF = 3584
TOP = 2
TOK_DEV = 256
MOE_TOK = 128
TOKENS = 2048
EXPERTS = 8
CAP = 64
MOE_TOTAL = 1024
N_EP = 8
N_TP = 4


def draw_log_decay(key, part):
    streams = jax.random.split(key, 7)
    ranking = jax.random.permutation(streams[0], HEADS)
    fast_heads = ranking < HEADS // 2
    quick = jnp.exp(jax.random.uniform(streams[1], (HEADS,), jnp.float32, jnp.log(3.0), jnp.log(8.0))) / TOK_DEV
    gentle = jnp.exp(jax.random.uniform(streams[2], (HEADS,), jnp.float32, jnp.log(0.03), jnp.log(0.25))) / TOKENS
    fading_speeds = jnp.where(fast_heads, quick, gentle)
    blocks = TOKENS // TOK_DEV
    multiplier_coefficient = jnp.exp(jax.random.uniform(streams[3], (blocks,), jnp.float32, jnp.log(0.5), jnp.log(2.0)))
    multiplier_coefficient = jnp.repeat(multiplier_coefficient, TOK_DEV)
    approximate_guess = jnp.exp(jax.random.uniform(streams[4], (TOKENS, HEADS), jnp.float32, -0.5, 0.5))
    word_slot_spots = jax.random.randint(streams[5], (2, HEADS), 0, TOKENS)
    stack_level_count = jax.random.uniform(streams[6], (2, HEADS), jnp.float32, jnp.log(0.6), jnp.log(0.85))
    sequence_offsets = jnp.arange(TOKENS, dtype=jnp.int32)[:, None, None]
    spike_clusters = jnp.sum(jnp.where(sequence_offsets == word_slot_spots[None], stack_level_count[None], 0.0), axis=1)
    return -(fading_speeds[None, :] * multiplier_coefficient[:, None] * approximate_guess) + spike_clusters


def raised(values, stream_key, source, target, parts, factor):
    owner, partner = [(jnp.arange(values.shape[position]) // (values.shape[position] // parts)).reshape([-1 if axis == position else 1 for axis in range(values.ndim)]) for position in (source, target)]
    chosen = jax.random.permutation(stream_key, parts)[partner]
    strong = (owner == chosen) | (owner == (partner + parts // 2) % parts)
    return jnp.where(strong, factor * values, values)


def levels(stream_key, shape, cuts, low, high):
    level, own = 1.0, jax.random.fold_in(stream_key, 6)
    for position, parts in cuts:
        draws = jnp.exp(jax.random.uniform(jax.random.fold_in(own, position), (parts,), jnp.float32, low / len(cuts), high / len(cuts)))
        level = level * jnp.repeat(draws, shape[position] // parts).reshape([-1 if axis == position else 1 for axis in range(len(shape))])
    return level


def assign_block(key, own, number, rows, amount, top, bound, lean):
    order = jax.random.permutation(key, amount)
    packed, ordinary = load_shares(amount, rows * top, bound, lean, True), load_shares(amount, rows * top, bound, lean, False)
    places = jnp.arange(amount)

    def named(tallies, rotation):
        used = int((tallies > 0).sum())
        fixed = max(1, used // 4)
        passed = fixed + (places - fixed + rotation * (used - fixed)) % max(1, amount - fixed)
        return jnp.zeros((amount,), jnp.int32).at[order[jnp.where(places < fixed, places, passed)]].set(jnp.asarray(tallies, jnp.int32))

    tallies = jnp.where(number % 4 == 0, named(packed, number // 4), named(ordinary, number - number // 4 - 1))
    mixed = jax.random.permutation(jax.random.fold_in(own, 3), amount)
    source_of, sink = mixed[0:amount // 2 * 2:2], mixed[1:amount // 2 * 2:2]
    room = jnp.minimum(tallies[source_of] - 1, bound - tallies[sink]) // 2
    room = jnp.where((source_of == order[0]) | (sink == order[0]) | (tallies[sink] == 0), 0, jnp.maximum(room, 0))
    passed = jax.random.randint(jax.random.fold_in(own, 4), (amount // 2,), 0, 1 << 20) % (room + 1)
    tallies = tallies.at[source_of].add(-passed).at[sink].add(passed)
    members = jnp.searchsorted(jnp.cumsum(tallies), jnp.arange(rows * top), side="right").astype(jnp.int32)
    table = members.reshape(top, rows).T
    table = table[jax.random.permutation(jax.random.fold_in(own, 1), rows)]
    rotation = jax.random.randint(jax.random.fold_in(own, 2), (rows, 1), 0, top)
    return jnp.take_along_axis(table, (jnp.arange(top)[None, :] + rotation) % top, axis=1)


def load_shares(count, total, most, slope, full):
    loads = [(1 << 20) // math.isqrt(grade ** slope) + 1 for grade in range(1, count + 1)]
    largest = most if full else min(most, max(-(-total // count), total * loads[0] // sum(loads)))
    least = 1 if total - largest >= count - 1 else 0
    holding, rest = [largest] + [least] * (count - 1), total - largest - least * (count - 1)
    while rest > 0:
        free = [i for i in range(1, count) if holding[i] < largest] or [i for i in range(1, count) if holding[i] < most]
        mass, left = sum([loads[i] for i in free]), rest
        for i in free:
            more = min(most - holding[i], max(1, left * loads[i] // mass), rest)
            holding[i] = holding[i] + more
            rest = rest - more
    return np.array(holding)


def noise(key, dims, scale, most, cuts=(), kind=jnp.bfloat16):
    drawn = scale * jax.random.normal(key, dims, jnp.float32)
    if cuts:
        drawn = drawn * levels(key, dims, cuts, -0.22, 0.18)
    return jnp.clip(drawn, -most, most).astype(kind)


def noise_with(own_key, shape, width, most, pieces, heavy, held_as=jnp.bfloat16):
    entries = width * jax.random.normal(own_key, shape, jnp.float32)
    if pieces:
        entries = entries * levels(own_key, shape, pieces, -0.22, 0.18)
    return jnp.clip(raised(entries, jax.random.fold_in(own_key, 3), *heavy), -most, most).astype(held_as)


def setup_inputs(seed: int = 0) -> dict:
    streams_of = jax.random.split(jax.random.key(seed), 15)
    queries = noise(streams_of[0], (TOKENS, HEADS * HEAD), 1.0, 6.0, ((0, 8), (1, 4)))
    key_rows = noise(streams_of[1], (TOKENS, HEADS * HEAD), 1.0, 6.0, ((0, 8), (1, 4)))
    value_rows = noise(streams_of[2], (TOKENS, HEADS * HEAD), 1.0, 6.0, ((0, 8), (1, 4)))
    out_gate = noise(streams_of[3], (TOKENS, HEADS * HEAD), 1.0, 6.0, ((0, 8), (1, 4)))
    log_decay = draw_log_decay(jax.random.fold_in(streams_of[14], 71), 0)
    head_gain = jnp.clip(1.0 + 0.18 * jax.random.normal(streams_of[5], (HEADS, HEAD), jnp.float32), 0.1, 1.9)
    out_weight = noise(streams_of[6], (HEADS * HEAD, D), (HEADS * HEAD) ** -0.5, 0.1875, ((0, 4),))
    moe_input = noise(streams_of[7], (MOE_TOTAL, D), 1.0, 6.0, ((0, 8),))
    moe_gain = jnp.clip(1.0 + 0.18 * jax.random.normal(streams_of[8], (D,), jnp.float32), 0.1, 1.9)
    expert_gate = noise(streams_of[9], (EXPERTS, D, EFF), D ** -0.5, 0.125, ((0, 8), (2, 4)))
    expert_up = noise(streams_of[10], (EXPERTS, D, EFF), D ** -0.5, 0.125, ((0, 8), (2, 4)))
    expert_down = noise_with(streams_of[11], (EXPERTS, EFF, D), EFF ** -0.5, 0.125, ((0, 8), (1, 4)), (1, 2, 4, 2.0))
    route_ids_keys = jax.random.split(jax.random.fold_in(streams_of[12], 1), MOE_TOTAL // MOE_TOK)
    route_ids_turns = jax.random.permutation(jax.random.fold_in(streams_of[12], 3), MOE_TOTAL // MOE_TOK)
    route_ids = jax.vmap(lambda own, number: assign_block(jax.random.fold_in(streams_of[12], 2), own, number, MOE_TOK, EXPERTS, TOP, CAP, 2))(route_ids_keys, route_ids_turns).reshape((MOE_TOTAL, TOP))
    route_weights = jnp.clip(0.2 + 0.8 * jax.random.uniform(streams_of[13], (MOE_TOTAL, TOP), jnp.float32) ** levels(streams_of[13], (MOE_TOTAL, TOP), ((0, 8),), -0.2, 0.2), 0.2, 1.0)
    return {"queries": queries, "key_rows": key_rows, "value_rows": value_rows, "out_gate": out_gate, "log_decay": log_decay, "head_gain": head_gain, "out_weight": out_weight, "moe_input": moe_input, "moe_gain": moe_gain, "expert_gate": expert_gate, "expert_up": expert_up, "expert_down": expert_down, "route_ids": route_ids, "route_weights": route_weights}


epsilon = 1e-06

def retention_block(state, inputs):
    query_heads, key_heads, value_heads, decay_block = inputs
    query_f = query_heads.astype(jnp.float32)
    key_f = key_heads.astype(jnp.float32)
    value_f = value_heads.astype(jnp.float32)
    cumulative = jnp.cumsum(decay_block, axis=0)
    block_total = cumulative[-1]
    scores = jnp.einsum('thd,shd->hts', query_f, key_f) * HEAD ** (-0.5)
    level = cumulative.T
    causal = jnp.arange(TOK_DEV, dtype=jnp.int32)[:, None] >= jnp.arange(TOK_DEV, dtype=jnp.int32)[None, :]
    spread = jnp.where(causal[None], level[:, :, None] - level[:, None, :], -jnp.inf)
    weights = (scores * jnp.exp(spread)).astype(jnp.bfloat16)
    inner = jnp.einsum('hts,shd->thd', weights.astype(jnp.float32), value_f)
    carried = jnp.einsum('thd,hde->the', query_f * jnp.exp(cumulative)[:, :, None], state, precision=lax.Precision.HIGHEST)
    scaled_keys = key_f * jnp.exp(block_total[None, :] - cumulative)[:, :, None]
    fresh = jnp.einsum('thd,the->hde', scaled_keys, value_f, precision=lax.Precision.HIGHEST)
    new_state = jnp.exp(block_total)[:, None, None] * state + fresh
    return (new_state, inner + carried)

def retention_ref(queries, key_rows, value_rows, out_gate, log_decay, head_gain, out_weight):
    blocks = TOKENS // TOK_DEV
    shaped = (blocks, TOK_DEV, HEADS, HEAD)
    start = jnp.zeros((HEADS, HEAD, HEAD), jnp.float32)
    _, retained = lax.scan(retention_block, start, (queries.reshape(shaped), key_rows.reshape(shaped), value_rows.reshape(shaped), log_decay.reshape(blocks, TOK_DEV, HEADS)))
    retained = retained.reshape(TOKENS, HEADS, HEAD)
    normed = retained * lax.rsqrt(lax.optimization_barrier(jnp.mean(retained * retained, axis=-1, keepdims=True)) + epsilon) * head_gain[None]
    gated = normed * jax.nn.silu(out_gate.reshape(TOKENS, HEADS, HEAD).astype(jnp.float32))
    heads_out = gated.reshape(TOKENS, HEADS * HEAD).astype(jnp.bfloat16)
    group = HEADS * HEAD // N_TP
    summed = jnp.zeros((TOKENS, D), jnp.float32)
    for member in range(N_TP):
        partial_sum = jnp.dot(heads_out[:, member * group:(member + 1) * group], out_weight[member * group:(member + 1) * group], preferred_element_type=jnp.float32).astype(jnp.bfloat16)
        summed = summed + lax.optimization_barrier(partial_sum).astype(jnp.float32)
    return summed.astype(jnp.bfloat16)

def slot_targets(block_ids):
    flat_ids = block_ids.reshape(-1)
    member = (flat_ids[:, None] == jnp.arange(EXPERTS, dtype=jnp.int32)[None, :]).astype(jnp.int32)
    ranks = lax.optimization_barrier(jnp.sum(jnp.cumsum(member, axis=0) * member, axis=1)) - 1
    return flat_ids * CAP + ranks

def experts_ref(moe_input, moe_gain, expert_gate, expert_up, expert_down, route_ids, route_weights):
    rows_f = moe_input.astype(jnp.float32)
    normed = (rows_f * lax.rsqrt(lax.optimization_barrier(jnp.mean(rows_f * rows_f, axis=-1, keepdims=True)) + epsilon) * moe_gain[None]).astype(jnp.bfloat16)
    pairs = MOE_TOK * TOP
    targets = jax.vmap(slot_targets)(route_ids.reshape(N_EP, MOE_TOK, TOP))
    pair_weights = route_weights.reshape(N_EP, pairs)
    block_index = jnp.arange(N_EP, dtype=jnp.int32)[:, None]
    group = EFF // N_TP

    def one_expert(total, expert):
        wanted = targets // CAP == expert
        local_slot = jnp.where(wanted, targets % CAP, CAP).astype(jnp.int32)
        table = jnp.full((N_EP, CAP + 1), pairs, jnp.int32)
        table = table.at[block_index, local_slot].set(jnp.arange(pairs, dtype=jnp.int32)[None, :])[:, :CAP]
        filled = table < pairs
        pair_index = jnp.minimum(table, pairs - 1)
        token_index = block_index * MOE_TOK + pair_index // TOP
        rows = jnp.where(filled[:, :, None], normed[token_index], jnp.zeros((), jnp.bfloat16)).reshape(N_EP * CAP, D)
        gate_w = lax.dynamic_index_in_dim(expert_gate, expert, 0, keepdims=False)
        up_w = lax.dynamic_index_in_dim(expert_up, expert, 0, keepdims=False)
        down_w = lax.dynamic_index_in_dim(expert_down, expert, 0, keepdims=False)
        hidden = (jax.nn.silu(jnp.dot(rows, gate_w, preferred_element_type=jnp.float32)) * jnp.dot(rows, up_w, preferred_element_type=jnp.float32)).astype(jnp.bfloat16)
        summed = jnp.zeros((N_EP * CAP, D), jnp.float32)
        for member in range(N_TP):
            partial_sum = jnp.dot(hidden[:, member * group:(member + 1) * group], down_w[member * group:(member + 1) * group], preferred_element_type=jnp.float32).astype(jnp.bfloat16)
            summed = summed + lax.optimization_barrier(partial_sum).astype(jnp.float32)
        results = summed.astype(jnp.bfloat16).astype(jnp.float32)
        scale = jnp.where(filled, jnp.take_along_axis(pair_weights, pair_index, axis=1), 0.0)
        contrib = scale.reshape(-1)[:, None] * results
        total = total.at[token_index.reshape(-1)].add(contrib)
        return (total, None)
    start = jnp.zeros((MOE_TOTAL, D), jnp.float32)
    total, _ = lax.scan(one_expert, start, jnp.arange(EXPERTS, dtype=jnp.int32))
    return total.astype(jnp.bfloat16)

def reference(queries, key_rows, value_rows, out_gate, log_decay, head_gain, out_weight, moe_input, moe_gain, expert_gate, expert_up, expert_down, route_ids, route_weights):
    mixer_out = retention_ref(queries, key_rows, value_rows, out_gate, log_decay, head_gain, out_weight)
    expert_out = experts_ref(moe_input, moe_gain, expert_gate, expert_up, expert_down, route_ids, route_weights)
    return (mixer_out, expert_out)
```

```python
import functools

import jax
import jax.numpy as jnp
from jax import lax
from jax.experimental import pallas as pl
from jax.experimental.pallas import tpu as pltpu
from jax.sharding import PartitionSpec as P

epsilon = 1e-06
CHUNKS = 2
BF = jnp.bfloat16
F32 = jnp.float32


def dot(a, b, dims=(((1,), (0,)), ((), ()))):
    return lax.dot_general(a, b, dims, preferred_element_type=F32)


def layer_kernel(
    n, cap, heads,
    q_ref, k_ref, v_ref, g_ref, cum_ref, cum_t_ref, gain_ref, piece_ref, hi_ref, lo_ref,
    ow_hbm, wg_hbm, wu_hbm, wd_hbm,
    mixer_ref, expert_ref,
    ow, wg, wu, wd, x, part, near, half, far, done, back,
    st, st_in, tot, tot_in, inner, ho, mx, mr1, ms, mr2,
    w_sem, own_sem, disp_s, disp_r, st_s, st_r, tot_s, tot_r, fwd_s, fwd_r,
    red_s, red_r, mix_s, mix_r, ret_s, ret_r,
):
    i, j = lax.axis_index("ep"), lax.axis_index("tp")
    j1 = j + 1 - 2 * lax.rem(j, 2)
    j2 = lax.rem(j + 2, 4)
    j3 = lax.rem(j1 + 2, 4)
    places = (j, j1, j2, j3)
    rows = n * cap
    step = rows // CHUNKS
    width = x.shape[2]
    dim = gain_ref.shape[1]
    length = q_ref.shape[0]
    quarter = length // 4

    def ahead(d):
        return lax.rem(i + d, n)

    def behind(d):
        return lax.rem(i + n - d, n)

    def send(src, dst, ss, rs, dev):
        return pltpu.make_async_remote_copy(
            src_ref=src, dst_ref=dst, send_sem=ss, recv_sem=rs, device_id=dev,
            device_id_type=pl.DeviceIdType.MESH,
        )

    loads = [
        pltpu.make_async_copy(a, b, w_sem.at[m])
        for m, (a, b) in enumerate(((ow_hbm, ow), (wg_hbm, wg), (wu_hbm, wu), (wd_hbm, wd)))
    ]
    for c in loads:
        c.start()
    own = pltpu.make_async_copy(piece_ref.at[pl.ds(0, cap)], x.at[0, pl.ds(0, cap)], own_sem.at[0])
    own.start()

    barrier = pltpu.get_barrier_semaphore()
    for d in range(1, n):
        pl.semaphore_signal(barrier, inc=1, device_id=(ahead(d), j), device_id_type=pl.DeviceIdType.MESH)
    for peer in (j1, j2):
        pl.semaphore_signal(barrier, inc=1, device_id=(i, peer), device_id_type=pl.DeviceIdType.MESH)
    pl.semaphore_wait(barrier, n + 1)

    sent = []
    disp = [None] * n
    for d in range(1, n):
        r = pl.ds(d * cap, cap)
        disp[d] = send(piece_ref.at[r], x.at[0, r], disp_s.at[d], disp_r.at[d], (ahead(d), j))
        disp[d].start()
        sent.append(disp[d])

    tot[...] = jnp.zeros_like(tot)
    for h in range(heads):
        c = slice(h * dim, (h + 1) * dim)
        total = cum_ref[length - 1 : length, h : h + 1]
        keys = k_ref[:, c].astype(F32) * jnp.exp(total - cum_ref[:, h : h + 1])
        st[h * dim : (h + 1) * dim, :] = dot(keys.T.astype(BF), v_ref[:, c]).astype(BF)
        tot[h : h + 1, :] = jnp.broadcast_to(total, (1, dim))
    st_c, tot_c = [None] * n, [None] * n
    for d in range(1, n):
        st_c[d] = send(st, st_in.at[d], st_s.at[d], st_r.at[d], (ahead(d), j))
        tot_c[d] = send(tot, tot_in.at[d], tot_s.at[d], tot_r.at[d], (ahead(d), j))

        @pl.when(i + d < n)
        def _():
            st_c[d].start()
            tot_c[d].start()

    y_c, c0_c, c2_c = [], [], []
    for g in range(CHUNKS):
        r = pl.ds(g * step, step)
        y_c.append(send(x.at[0, r], x.at[2, r], fwd_s.at[g, 0], fwd_r.at[g, 0], (i, j2)))
        c0_c.append(send(x.at[0, r], x.at[1, r], fwd_s.at[g, 1], fwd_r.at[g, 1], (i, j1)))
        c2_c.append(send(x.at[2, r], x.at[3, r], fwd_s.at[g, 2], fwd_r.at[g, 2], (i, j1)))
    sent += y_c + c0_c + c2_c

    def forward(g):
        for d in range(g * (n // CHUNKS), (g + 1) * (n // CHUNKS)):
            if d == 0:
                own.wait()
            else:
                disp[d].wait_recv()
        y_c[g].start()
        c0_c[g].start()

    def relay(g):
        y_c[g].wait_recv()
        c2_c[g].start()

    forward(0)

    causal = lax.broadcasted_iota(jnp.int32, (length, length), 0) >= lax.broadcasted_iota(
        jnp.int32, (length, length), 1
    )
    for h in range(heads):
        c = slice(h * dim, (h + 1) * dim)
        scores = dot(q_ref[:, c], k_ref[:, c], (((1,), (1,)), ((), ()))) * dim ** (-0.5)
        spread = jnp.where(causal, cum_ref[:, h : h + 1] - cum_t_ref[h : h + 1, :], -jnp.inf)
        inner[:, c] = dot((scores * jnp.exp(spread)).astype(BF), v_ref[:, c])

    for g in range(1, CHUNKS):
        forward(g)
    relay(0)

    entering = jnp.zeros((heads * dim, dim), F32)
    for d in range(n - 1, 0, -1):
        @pl.when(i >= d)
        def _():
            st_c[d].wait_recv()
            tot_c[d].wait_recv()

        @pl.when(i < d)
        def _():
            st_in[d] = jnp.zeros(st_in.shape[1:], BF)
            tot_in[d] = jnp.zeros(tot_in.shape[1:], F32)

        decay = jnp.concatenate(
            [jnp.broadcast_to(jnp.exp(tot_in[d, h : h + 1, :]), (dim, dim)) for h in range(heads)], axis=0
        )
        entering = decay * entering + st_in[d].astype(F32)
    entering = entering.astype(BF)
    for h in range(heads):
        c = slice(h * dim, (h + 1) * dim)
        queries = (q_ref[:, c].astype(F32) * jnp.exp(cum_ref[:, h : h + 1])).astype(BF)
        kept = inner[:, c] + dot(queries, entering[h * dim : (h + 1) * dim, :])
        normed = kept * lax.rsqrt(jnp.mean(kept * kept, axis=-1, keepdims=True) + epsilon)
        ho[:, c] = (normed * gain_ref[h : h + 1, :] * jax.nn.silu(g_ref[:, c].astype(F32))).astype(BF)
    loads[0].wait()
    mx[...] = dot(ho[...], ow[...]).astype(BF)

    def stripe(m):
        return pl.ds(pl.multiple_of(places[m] * quarter, quarter), quarter)

    mix_a = send(mx.at[stripe(1)], mr1.at[0], mix_s.at[0], mix_r.at[0], (i, j1))
    mix_b = send(mx.at[stripe(3)], mr1.at[1], mix_s.at[1], mix_r.at[1], (i, j1))
    mix_c = send(ms, mr2, mix_s.at[2], mix_r.at[2], (i, j2))
    mix_b.start()
    mix_a.start()
    sent += [mix_a, mix_b, mix_c]
    for g in range(1, CHUNKS):
        relay(g)
    for c in loads[1:]:
        c.wait()

    red = []
    for g in range(CHUNKS):
        r = pl.ds(g * step, step)
        red.append((
            send(part.at[1, r], near.at[0, r], red_s.at[g, 0], red_r.at[g, 0], (i, j1)),
            send(part.at[3, r], near.at[1, r], red_s.at[g, 1], red_r.at[g, 1], (i, j1)),
            send(half.at[r], far.at[r], red_s.at[g, 2], red_r.at[g, 2], (i, j2)),
        ))
        sent += list(red[-1])

    def block(m):
        return pl.ds(pl.multiple_of(places[m] * width, width), width)

    def experts(g):
        r = pl.ds(g * step, step)
        gate, up = 0.0, 0.0
        for m in (0, 2, 1, 3):
            if m == 1:
                c0_c[g].wait_recv()
                c2_c[g].wait_recv()
            gate = gate + dot(x[m, r, :], wg[block(m), :])
            up = up + dot(x[m, r, :], wu[block(m), :])
        hidden = (jax.nn.silu(gate) * up).astype(BF)
        for m in (3, 1, 2, 0):
            part[m, r, :] = dot(hidden, wd[:, block(m)]).astype(BF)
            if m == 3:
                red[g][1].start()
            if m == 1:
                red[g][0].start()

    def cross(g):
        r = pl.ds(g * step, step)
        red[g][1].wait_recv()
        half[r, :] = (part[2, r, :].astype(F32) + near[1, r, :].astype(F32)).astype(BF)
        red[g][2].start()

    ret = [None] * n
    for d in range(n):
        r = pl.ds(d * cap, cap)
        if d:
            ret[d] = send(done.at[r], back.at[r], ret_s.at[d], ret_r.at[d], (behind(d), j))
            sent.append(ret[d])

    def home(g):
        r = pl.ds(g * step, step)
        red[g][0].wait_recv()
        red[g][2].wait_recv()
        done[r, :] = (
            part[0, r, :].astype(F32) + near[0, r, :].astype(F32) + far[r, :].astype(F32)
        ).astype(BF)
        for d in range(g * (n // CHUNKS), (g + 1) * (n // CHUNKS)):
            if d:
                ret[d].start()
        if g == 0:
            back[pl.ds(0, cap), :] = done[pl.ds(0, cap), :]

    experts(0)
    cross(0)
    mix_b.wait_recv()
    ms[...] = (mx[stripe(2), :].astype(F32) + mr1[1].astype(F32)).astype(BF)
    mix_c.start()
    for g in range(1, CHUNKS):
        experts(g)
        home(g - 1)
        cross(g)
    mix_a.wait_recv()
    mix_c.wait_recv()
    mixer_ref[...] = (
        mx[stripe(0), :].astype(F32) + mr1[0].astype(F32) + mr2[...].astype(F32)
    ).astype(BF)
    home(CHUNKS - 1)
    for d in range(1, n):
        ret[d].wait_recv()
    expert_ref[...] = (dot(hi_ref[...], back[...]) + dot(lo_ref[...], back[...])).astype(BF)
    for c in sent:
        c.wait_send()
    for d in range(1, n):
        @pl.when(i + d < n)
        def _():
            st_c[d].wait_send()
            tot_c[d].wait_send()


def per_device(
    queries, key_rows, value_rows, out_gate, log_decay, head_gain, out_weight,
    moe_input, moe_gain, expert_gate, expert_up, expert_down, route_ids, route_weights,
):
    n, shares = lax.axis_size("ep"), lax.axis_size("tp")
    i, j = lax.axis_index("ep"), lax.axis_index("tp")
    tokens, top = route_ids.shape
    pairs = tokens * top
    cap = -(-2 * pairs // n // 16) * 16
    full = moe_input.shape[1]
    width = full // shares
    length, heads = log_decay.shape
    dim = head_gain.shape[1]
    hidden = expert_gate.shape[2]

    rows_f = moe_input.astype(F32)
    scale = lax.rsqrt(jnp.mean(rows_f * rows_f, axis=-1, keepdims=True) + epsilon)
    mine = lax.dynamic_slice_in_dim(moe_input, j * width, width, 1).astype(F32)
    gain = lax.dynamic_slice_in_dim(moe_gain, j * width, width, 0)
    normed = (mine * scale * gain[None]).astype(BF)

    flat = route_ids.reshape(-1)
    member = flat[:, None] == jnp.arange(n, dtype=jnp.int32)[None, :]
    lower = jnp.arange(pairs)[:, None] >= jnp.arange(pairs)[None, :]
    counts = jnp.dot(lower.astype(BF), member.astype(BF), preferred_element_type=F32)
    ranks = jnp.sum(jnp.where(member, counts, 0.0), axis=1).astype(jnp.int32) - 1
    targets = (lax.rem(flat - i + n, n) * cap + ranks).reshape(tokens, top)
    slots = jnp.arange(n * cap, dtype=jnp.int32)
    pick = sum(((targets[:, t][None, :] == slots[:, None]).astype(BF) for t in range(top)))
    piece = jnp.dot(pick, normed, preferred_element_type=F32).astype(BF)
    comb = sum(
        jnp.where(targets[:, t][:, None] == slots[None, :], route_weights[:, t][:, None], 0.0)
        for t in range(top)
    )
    hi = lax.reduce_precision(comb, 8, 7)
    lo = (comb - hi).astype(BF)
    hi = hi.astype(BF)
    cum = jnp.cumsum(log_decay, axis=0)

    rows = n * cap
    quarter = length // shares
    vmem = pl.BlockSpec(memory_space=pltpu.VMEM)
    hbm = pl.BlockSpec(memory_space=pl.ANY)
    dma = pltpu.SemaphoreType.DMA
    return pl.pallas_call(
        functools.partial(layer_kernel, n, cap, heads),
        out_shape=(
            jax.ShapeDtypeStruct((quarter, full), BF),
            jax.ShapeDtypeStruct((tokens, width), BF),
        ),
        in_specs=[vmem] * 10 + [hbm] * 4,
        out_specs=(vmem, vmem),
        scratch_shapes=[
            pltpu.VMEM(out_weight.shape, BF),
            pltpu.VMEM((full, hidden), BF),
            pltpu.VMEM((full, hidden), BF),
            pltpu.VMEM((hidden, full), BF),
            pltpu.VMEM((4, rows, width), BF),
            pltpu.VMEM((4, rows, width), BF),
            pltpu.VMEM((2, rows, width), BF),
            pltpu.VMEM((rows, width), BF),
            pltpu.VMEM((rows, width), BF),
            pltpu.VMEM((rows, width), BF),
            pltpu.VMEM((rows, width), BF),
            pltpu.VMEM((heads * dim, dim), BF),
            pltpu.VMEM((n, heads * dim, dim), BF),
            pltpu.VMEM((8, dim), F32),
            pltpu.VMEM((n, 8, dim), F32),
            pltpu.VMEM((length, heads * dim), F32),
            pltpu.VMEM((length, heads * dim), BF),
            pltpu.VMEM((length, full), BF),
            pltpu.VMEM((2, quarter, full), BF),
            pltpu.VMEM((quarter, full), BF),
            pltpu.VMEM((quarter, full), BF),
            dma((4,)), dma((1,)),
            dma((n,)), dma((n,)), dma((n,)), dma((n,)), dma((n,)), dma((n,)),
            dma((CHUNKS, 3)), dma((CHUNKS, 3)),
            dma((CHUNKS, 3)), dma((CHUNKS, 3)),
            dma((3,)), dma((3,)),
            dma((n,)), dma((n,)),
        ],
        compiler_params=pltpu.CompilerParams(
            collective_id=0, has_side_effects=True, vmem_limit_bytes=60 * 1024 * 1024
        ),
    )(
        queries, key_rows, value_rows, out_gate, cum, cum.T, head_gain, piece, hi, lo,
        out_weight, expert_gate[0], expert_up[0], expert_down[0],
    )


def solution(mesh):
    in_specs = (
        P("ep", "tp"),
        P("ep", "tp"),
        P("ep", "tp"),
        P("ep", "tp"),
        P("ep", "tp"),
        P("tp", None),
        P("tp", None),
        P("ep", None),
        P(),
        P("ep", None, "tp"),
        P("ep", None, "tp"),
        P("ep", "tp", None),
        P("ep", None),
        P("ep", None),
    )
    out_specs = (P(("ep", "tp"), None), P("ep", "tp"))
    return jax.shard_map(
        per_device, mesh=mesh, in_specs=in_specs, out_specs=out_specs, check_vma=False
    )
```

```python
import functools

import jax
import jax.numpy as jnp
from jax import lax
from jax.experimental import pallas as pl
from jax.experimental.pallas import tpu as pltpu
from jax.sharding import PartitionSpec as P

epsilon = 1e-06
CHUNKS = 2
PARTS = 2
BF = jnp.bfloat16
F32 = jnp.float32


def dot(a, b, dims=(((1,), (0,)), ((), ()))):
    return lax.dot_general(a, b, dims, preferred_element_type=F32)


def layer_kernel(
    n, cap, heads,
    q_ref, k_ref, v_ref, g_ref, ld_ref, gain_ref, tok_ref, norm_ref, ids_ref, rw_ref,
    ow_hbm, wg_hbm, wu_hbm, wd_hbm,
    mixer_ref, expert_ref,
    ow, wg, wu, wd, x, part, near, half, far, done, back,
    st, st_in, tot, tot_in, inner, ho, mx, mr1, ms, mr2,
    w_sem, disp_s, disp_r, st_s, st_r, tot_s, tot_r, fwd_s, fwd_r,
    red_s, red_r, redy_s, redy_r, mix_s, mix_r, ret_s, ret_r,
    piece_ref, hi_ref, lo_ref,
):
    i, j = lax.axis_index("ep"), lax.axis_index("tp")
    j1 = j + 1 - 2 * lax.rem(j, 2)
    j2 = lax.rem(j + 2, 4)
    j3 = lax.rem(j1 + 2, 4)
    places = (j, j1, j2, j3)
    rows = n * cap
    step = rows // CHUNKS
    width = x.shape[2]
    dim = gain_ref.shape[1]
    length = q_ref.shape[0]
    quarter = length // 4

    def shift(p):
        return (p + 1) // 2 if p % 2 else n - p // 2

    def ahead(p):
        return lax.rem(i + shift(p), n)

    def behind(p):
        return lax.rem(i + n - shift(p), n)

    def send(src, dst, ss, rs, dev):
        return pltpu.make_async_remote_copy(
            src_ref=src, dst_ref=dst, send_sem=ss, recv_sem=rs, device_id=dev,
            device_id_type=pl.DeviceIdType.MESH,
        )

    loads = [
        pltpu.make_async_copy(a, b, w_sem.at[m])
        for m, (a, b) in enumerate(((ow_hbm, ow), (wg_hbm, wg), (wu_hbm, wu), (wd_hbm, wd)))
    ]
    for c in loads:
        c.start()
    barrier = pltpu.get_barrier_semaphore()
    for d in range(1, n):
        pl.semaphore_signal(barrier, inc=1, device_id=(ahead(d), j), device_id_type=pl.DeviceIdType.MESH)
    for peer in (j1, j2):
        pl.semaphore_signal(barrier, inc=1, device_id=(i, peer), device_id_type=pl.DeviceIdType.MESH)

    tokens, top = ids_ref.shape
    lanes = -(-n // 128) * 128
    rows_f = tok_ref[...].astype(F32)
    scale = lax.rsqrt(jnp.mean(rows_f * rows_f, axis=-1, keepdims=True) + epsilon)
    mine = pl.ds(pl.multiple_of(j * width, width), width)
    normed = (tok_ref[:, mine].astype(F32) * scale * norm_ref[:, mine]).astype(BF)
    expert = lax.broadcasted_iota(jnp.int32, (tokens, lanes), 1)
    named = [ids_ref[:, t : t + 1] == expert for t in range(top)]
    strict = lax.broadcasted_iota(jnp.int32, (tokens, tokens), 0) > lax.broadcasted_iota(
        jnp.int32, (tokens, tokens), 1
    )
    held = sum(jnp.where(m, 1.0, 0.0) for m in named)
    before = dot(jnp.where(strict, 1.0, 0.0).astype(BF), held.astype(BF))
    slot = lax.broadcasted_iota(jnp.int32, (tokens, rows), 1)
    pick, comb = 0.0, 0.0
    for t in range(top):
        rank = jnp.sum(jnp.where(named[t], before, 0.0), axis=1, keepdims=True).astype(jnp.int32)
        d = ids_ref[:, t : t + 1] - i
        d = jnp.where(d < 0, d + n, d)
        place = jnp.where(d == 0, 0, jnp.where(2 * d <= n, 2 * d - 1, 2 * (n - d)))
        hit = slot == place * cap + rank
        pick = pick + jnp.where(hit, 1.0, 0.0)
        comb = comb + jnp.where(hit, rw_ref[:, t : t + 1], 0.0)
    piece = dot(pick.T.astype(BF), normed).astype(BF)
    piece_ref[...] = piece
    x[0, 0:cap, :] = piece[0:cap]
    pl.semaphore_wait(barrier, n + 1)

    sent = []
    disp = [None] * n
    for d in range(1, n):
        r = pl.ds(d * cap, cap)
        disp[d] = send(piece_ref.at[r], x.at[0, r], disp_s.at[d], disp_r.at[d], (ahead(d), j))
        disp[d].start()
        sent.append(disp[d])

    tot[...] = jnp.zeros_like(tot)
    hi = comb.astype(BF)
    hi_ref[...] = hi
    lo_ref[...] = (comb - hi.astype(F32)).astype(BF)
    causal = lax.broadcasted_iota(jnp.int32, (length, length), 0) >= lax.broadcasted_iota(
        jnp.int32, (length, length), 1
    )
    lower = jnp.where(causal, 1.0, 0.0)
    cum = [
        lax.dot_general(
            lower, jnp.broadcast_to(ld_ref[:, h : h + 1], (length, dim)), (((1,), (0,)), ((), ())),
            precision=lax.Precision.HIGHEST, preferred_element_type=F32,
        )
        for h in range(heads)
    ]

    for h in range(heads):
        c = slice(h * dim, (h + 1) * dim)
        total = cum[h][length - 1 : length, :]
        keys = k_ref[:, c].astype(F32) * jnp.exp(total - cum[h])
        st[h * dim : (h + 1) * dim, :] = dot(keys.T.astype(BF), v_ref[:, c]).astype(BF)
        tot[h : h + 1, :] = total
    st_c, tot_c = [None] * n, [None] * n
    for d in range(1, n):
        later = (lax.rem(i + d, n), j)
        st_c[d] = send(st, st_in.at[d], st_s.at[d], st_r.at[d], later)
        tot_c[d] = send(tot, tot_in.at[d], tot_s.at[d], tot_r.at[d], later)

    y_c, c0_c, c2_c = [], [], []
    small = step // PARTS
    group = n // (CHUNKS * PARTS)
    for u in range(CHUNKS * PARTS):
        r = pl.ds(u * small, small)
        y_c.append(send(x.at[0, r], x.at[2, r], fwd_s.at[u, 0], fwd_r.at[u, 0], (i, j2)))
        c0_c.append(send(x.at[0, r], x.at[1, r], fwd_s.at[u, 1], fwd_r.at[u, 1], (i, j1)))
        c2_c.append(send(x.at[2, r], x.at[3, r], fwd_s.at[u, 2], fwd_r.at[u, 2], (i, j1)))
    sent += y_c + c0_c + c2_c

    def forward(u):
        for d in range(max(1, u * group), (u + 1) * group):
            disp[d].wait_recv()
        y_c[u].start()
        c0_c[u].start()

    def relay(u):
        y_c[u].wait_recv()
        c2_c[u].start()

    for u in range(PARTS):
        forward(u)
    for d in range(1, n):
        @pl.when(i + d < n)
        def _():
            st_c[d].start()
            tot_c[d].start()

    for h in range(heads):
        c = slice(h * dim, (h + 1) * dim)
        scores = dot(q_ref[:, c], k_ref[:, c], (((1,), (1,)), ((), ()))) * dim ** (-0.5)
        spread = jnp.where(causal, cum[h][:, 0:1] - cum[h].T[0:1, :], -jnp.inf)
        inner[:, c] = dot((scores * jnp.exp(spread)).astype(BF), v_ref[:, c])

    for u in range(PARTS):
        forward(PARTS + u)
        relay(u)
    loads[0].wait()
    for c in loads[1:]:
        c.wait()

    def stripe(m):
        return pl.ds(pl.multiple_of(places[m] * quarter, quarter), quarter)

    mix_a = send(mx.at[stripe(1)], mr1.at[0], mix_s.at[0], mix_r.at[0], (i, j1))
    mix_b = send(mx.at[stripe(3)], mr1.at[1], mix_s.at[1], mix_r.at[1], (i, j1))
    mix_c = send(ms, mr2, mix_s.at[2], mix_r.at[2], (i, j2))
    sent += [mix_a, mix_b, mix_c]

    def retention():
        entering = jnp.zeros((heads * dim, dim), F32)
        for d in range(n - 1, 0, -1):
            @pl.when(i >= d)
            def _():
                st_c[d].wait_recv()
                tot_c[d].wait_recv()

            @pl.when(i < d)
            def _():
                st_in[d] = jnp.zeros(st_in.shape[1:], BF)
                tot_in[d] = jnp.zeros(tot_in.shape[1:], F32)

            decay = jnp.concatenate(
                [jnp.broadcast_to(jnp.exp(tot_in[d, h : h + 1, :]), (dim, dim)) for h in range(heads)], axis=0
            )
            entering = decay * entering + st_in[d].astype(F32)
        entering = entering.astype(BF)
        for h in range(heads):
            c = slice(h * dim, (h + 1) * dim)
            queries = (q_ref[:, c].astype(F32) * jnp.exp(cum[h])).astype(BF)
            kept = inner[:, c] + dot(queries, entering[h * dim : (h + 1) * dim, :])
            normed = kept * lax.rsqrt(jnp.mean(kept * kept, axis=-1, keepdims=True) + epsilon)
            ho[:, c] = (normed * gain_ref[h : h + 1, :] * jax.nn.silu(g_ref[:, c].astype(F32))).astype(BF)
        mx[...] = dot(ho[...], ow[...]).astype(BF)

        mix_b.start()
        mix_a.start()

    red, red_y = [], []
    for g in range(CHUNKS):
        r = pl.ds(g * step, step)
        red.append((
            send(part.at[1, r], near.at[0, r], red_s.at[g, 0], red_r.at[g, 0], (i, j1)),
            send(part.at[3, r], near.at[1, r], red_s.at[g, 1], red_r.at[g, 1], (i, j1)),
        ))
        sent += list(red[-1])
    for u in range(CHUNKS * PARTS):
        r = pl.ds(u * small, small)
        red_y.append(send(half.at[r], far.at[r], redy_s.at[u], redy_r.at[u], (i, j2)))
    sent += red_y

    def block(m):
        return pl.ds(pl.multiple_of(places[m] * width, width), width)

    def experts(g, between):
        r = pl.ds(g * step, step)
        gate, up = 0.0, 0.0
        for m in (0, 2, 1, 3):
            if m == 1:
                for u in range(g * PARTS, (g + 1) * PARTS):
                    c0_c[u].wait_recv()
                    c2_c[u].wait_recv()
            gate = gate + dot(x[m, r, :], wg[block(m), :])
            up = up + dot(x[m, r, :], wu[block(m), :])
        hidden = (jax.nn.silu(gate) * up).astype(BF)
        between()
        for m in (3, 2, 1, 0):
            part[m, r, :] = dot(hidden, wd[:, block(m)]).astype(BF)
            if m == 3:
                red[g][1].start()
            if m == 1:
                red[g][0].start()
                cross(g)

    def cross(g):
        red[g][1].wait_recv()
        for u in range(g * PARTS, (g + 1) * PARTS):
            r = pl.ds(u * small, small)
            half[r, :] = (part[2, r, :].astype(F32) + near[1, r, :].astype(F32)).astype(BF)
            red_y[u].start()

    ret = [None] * n
    for d in range(n):
        r = pl.ds(d * cap, cap)
        if d:
            ret[d] = send(done.at[r], back.at[r], ret_s.at[d], ret_r.at[d], (behind(d), j))
            sent.append(ret[d])

    def home(g):
        red[g][0].wait_recv()
        for u in range(g * PARTS, (g + 1) * PARTS):
            r = pl.ds(u * small, small)
            red_y[u].wait_recv()
            done[r, :] = (
                part[0, r, :].astype(F32) + near[0, r, :].astype(F32) + far[r, :].astype(F32)
            ).astype(BF)
            for d in range(u * group, (u + 1) * group):
                if d:
                    ret[d].start()
                else:
                    back[pl.ds(0, cap), :] = done[pl.ds(0, cap), :]

    def mix_cross():
        mix_b.wait_recv()
        ms[...] = (mx[stripe(2), :].astype(F32) + mr1[1].astype(F32)).astype(BF)
        mix_c.start()

    experts(0, lambda: None)
    for u in range(PARTS, CHUNKS * PARTS):
        relay(u)
    retention()
    for g in range(1, CHUNKS):
        experts(g, mix_cross if g == 1 else lambda: None)
        home(g - 1)
    mix_a.wait_recv()
    mix_c.wait_recv()
    mixer_ref[...] = (
        mx[stripe(0), :].astype(F32) + mr1[0].astype(F32) + mr2[...].astype(F32)
    ).astype(BF)
    home(CHUNKS - 1)
    for d in range(1, n):
        ret[d].wait_recv()
    expert_ref[...] = (dot(hi_ref[...], back[...]) + dot(lo_ref[...], back[...])).astype(BF)
    for c in sent:
        c.wait_send()
    for d in range(1, n):
        @pl.when(i + d < n)
        def _():
            st_c[d].wait_send()
            tot_c[d].wait_send()


def store_kernel(mixer, blended, mixer_out, blended_out, sem):
    copies = [
        pltpu.make_async_copy(mixer, mixer_out, sem.at[0]),
        pltpu.make_async_copy(blended, blended_out, sem.at[1]),
    ]
    for c in copies:
        c.start()
    for c in copies:
        c.wait()


def per_device(
    queries, key_rows, value_rows, out_gate, log_decay, head_gain, out_weight,
    moe_input, moe_gain, expert_gate, expert_up, expert_down, route_ids, route_weights,
):
    n, shares = lax.axis_size("ep"), lax.axis_size("tp")
    tokens, top = route_ids.shape
    pairs = tokens * top
    cap = -(-2 * pairs // n // 16) * 16
    full = moe_input.shape[1]
    width = full // shares
    length, heads = log_decay.shape
    dim = head_gain.shape[1]
    hidden = expert_gate.shape[2]

    rows = n * cap
    quarter = length // shares
    vmem = pl.BlockSpec(memory_space=pltpu.VMEM)
    hbm = pl.BlockSpec(memory_space=pltpu.HBM)
    dma = pltpu.SemaphoreType.DMA
    mixer, blended = pl.pallas_call(
        functools.partial(layer_kernel, n, cap, heads),
        out_shape=(
            jax.ShapeDtypeStruct((quarter, full), BF),
            jax.ShapeDtypeStruct((tokens, width), BF),
        ),
        in_specs=[vmem] * 10 + [hbm] * 4,
        out_specs=(vmem, vmem),
        scratch_shapes=[
            pltpu.VMEM(out_weight.shape, BF),
            pltpu.VMEM((full, hidden), BF),
            pltpu.VMEM((full, hidden), BF),
            pltpu.VMEM((hidden, full), BF),
            pltpu.VMEM((4, rows, width), BF),
            pltpu.VMEM((4, rows, width), BF),
            pltpu.VMEM((2, rows, width), BF),
            pltpu.VMEM((rows, width), BF),
            pltpu.VMEM((rows, width), BF),
            pltpu.VMEM((rows, width), BF),
            pltpu.VMEM((rows, width), BF),
            pltpu.VMEM((heads * dim, dim), BF),
            pltpu.VMEM((n, heads * dim, dim), BF),
            pltpu.VMEM((8, dim), F32),
            pltpu.VMEM((n, 8, dim), F32),
            pltpu.VMEM((length, heads * dim), F32),
            pltpu.VMEM((length, heads * dim), BF),
            pltpu.VMEM((length, full), BF),
            pltpu.VMEM((2, quarter, full), BF),
            pltpu.VMEM((quarter, full), BF),
            pltpu.VMEM((quarter, full), BF),
            dma((4,)),
            dma((n,)), dma((n,)), dma((n,)), dma((n,)), dma((n,)), dma((n,)),
            dma((CHUNKS * PARTS, 3)), dma((CHUNKS * PARTS, 3)),
            dma((CHUNKS, 2)), dma((CHUNKS, 2)),
            dma((CHUNKS * PARTS,)), dma((CHUNKS * PARTS,)),
            dma((3,)), dma((3,)),
            dma((n,)), dma((n,)),
            pltpu.VMEM((rows, width), BF),
            pltpu.VMEM((tokens, rows), BF),
            pltpu.VMEM((tokens, rows), BF),
        ],
        compiler_params=pltpu.CompilerParams(
            collective_id=0, has_side_effects=True, vmem_limit_bytes=44 * 1024 * 1024
        ),
    )(
        queries, key_rows, value_rows, out_gate, log_decay, head_gain,
        moe_input, moe_gain.reshape(1, full), route_ids, route_weights,
        out_weight, expert_gate[0], expert_up[0], expert_down[0],
    )
    return pl.pallas_call(
        store_kernel,
        out_shape=(
            jax.ShapeDtypeStruct(mixer.shape, BF),
            jax.ShapeDtypeStruct(blended.shape, BF),
        ),
        in_specs=[vmem, vmem],
        out_specs=(hbm, hbm),
        scratch_shapes=[dma((2,))],
        compiler_params=pltpu.CompilerParams(vmem_limit_bytes=4 * 1024 * 1024),
    )(mixer, blended)


def solution(mesh):
    in_specs = (
        P("ep", "tp"),
        P("ep", "tp"),
        P("ep", "tp"),
        P("ep", "tp"),
        P("ep", "tp"),
        P("tp", None),
        P("tp", None),
        P("ep", None),
        P(),
        P("ep", None, "tp"),
        P("ep", None, "tp"),
        P("ep", "tp", None),
        P("ep", None),
        P("ep", None),
    )
    out_specs = (P(("ep", "tp"), None), P("ep", "tp"))
    return jax.shard_map(
        per_device, mesh=mesh, in_specs=in_specs, out_specs=out_specs, check_vma=False
    )
```
